32 devices in a mesh: grp: 2 (over x), ep: 8 (over z, y), tp: 2 (over core).
Axes of the slice: x: 2, y: 2, z: 4, core: 2. Of those that a mesh axis runs over, the one named last changes fastest.
Arguments:
- tokens: bfloat16 [4096, 2048], P(('grp', 'ep', 'tp')), parts along dimension 0, may hold values from -6 to 6
- norm_gain: float32 [2048], replicated, may hold values from 0.1 to 1.9
- expert_ids: int32 [4096, 2], P(('grp', 'ep', 'tp')), parts along dimension 0, may hold values from 0 to 7, all different within a row; in each aligned block of 128 rows (0 to 127, 128 to 255, ...) at most 64 rows name the same one
- route_weights: float32 [4096, 2], P(('grp', 'ep', 'tp')), parts along dimension 0, may hold values from 0.2 to 1
- gate_proj: bfloat16 [8, 2048, 1536], P('ep', None, 'tp'), may hold values from -0.375 to 0.375
- linear_proj: bfloat16 [8, 2048, 1536], P('ep', None, 'tp'), may hold values from -0.375 to 0.375
- down_proj: bfloat16 [8, 1536, 2048], P('ep', 'tp'), may hold values from -0.01953125 to 0.01953125
Outputs:
- mixed: bfloat16 [4096, 2048], P(('grp', 'ep', 'tp')), parts along dimension 0
The draws below stay inside these ranges and needn't reach their ends.
There are 2 independent parts, one for each index of `grp`. The reference program is written for one: setup_inputs(seed, part) draws one part's arguments, and reference() takes and returns one part's arrays. A program takes and returns all parts, laid end to end along the dimension named above; an argument that names none is the same for every part. Nothing has to cross between parts.
Inputs may be any that keep to these rules, and one draw needn't show every extreme that they name: `expert_ids`: each token names 2 different experts. Among the 128 rows of one device (aligned blocks) no expert is named more than 64 times, a bound that some expert reaches in some blocks.
All inputs are finite; a program needn't handle non-finite values.
Results may differ from the reference program's by a relative error of at most 0.009.
Values may be sent and summed in bfloat16 or wider, within the bound.
A program may use at most 64 MiB of HBM per device.

```python
import math
import jax
import jax.numpy as jnp
import numpy as np
from jax import lax

D = 2048
FF = 1536
TOK_DEV = 128
TOPK = 2
EXPERTS = 8
CAP = 64
TOKENS = 2048
N_EP = 8
N_TP = 2


def block_levels(key, extent, pieces, smallest, top_value):
    gain = 1.0
    for position, shards_of in pieces:
        heights = jax.random.uniform(jax.random.fold_in(jax.random.fold_in(key, 6), position), (shards_of,), jnp.float32, smallest / len(pieces), top_value / len(pieces))
        gain = gain * jnp.repeat(jnp.exp(heights), extent[position] // shards_of).reshape((-1,) + (1,) * (len(extent) - 1 - position))
    return gain


def shared_out(rng, own, number, rows, number_of, top, reach, lean):
    ranking = jax.random.permutation(rng, number_of)
    crowded, ordinary = portions_of(number_of, rows * top, reach, lean, True), portions_of(number_of, rows * top, reach, lean, False)
    places = jnp.arange(number_of)

    def named(tallies, turn):
        used = int((tallies > 0).sum())
        fixed = max(1, used // 4)
        shifted = fixed + (places - fixed + turn * (used - fixed)) % max(1, number_of - fixed)
        return jnp.zeros((number_of,), jnp.int32).at[ranking[jnp.where(places < fixed, places, shifted)]].set(jnp.asarray(tallies, jnp.int32))

    tallies = jnp.where(number % 4 == 0, named(crowded, number // 4), named(ordinary, number - number // 4 - 1))
    mixed = jax.random.permutation(jax.random.fold_in(own, 3), number_of)
    giver, taker = mixed[0:number_of // 2 * 2:2], mixed[1:number_of // 2 * 2:2]
    margin = jnp.minimum(tallies[giver] - 1, reach - tallies[taker]) // 2
    margin = jnp.where((giver == ranking[0]) | (taker == ranking[0]) | (tallies[taker] == 0), 0, jnp.maximum(margin, 0))
    shifted = jax.random.randint(jax.random.fold_in(own, 4), (number_of // 2,), 0, 1 << 20) % (margin + 1)
    tallies = tallies.at[giver].add(-shifted).at[taker].add(shifted)
    labels = jnp.searchsorted(jnp.cumsum(tallies), jnp.arange(rows * top), side="right").astype(jnp.int32)
    grid = labels.reshape(top, rows).T
    grid = grid[jax.random.permutation(jax.random.fold_in(own, 1), rows)]
    turn = jax.random.randint(jax.random.fold_in(own, 2), (rows, 1), 0, top)
    return jnp.take_along_axis(grid, (jnp.arange(top)[None, :] + turn) % top, axis=1)


def portions_of(count, total, reach, skew, full):
    weights = [(1 << 20) // math.isqrt(grade ** skew) + 1 for grade in range(1, count + 1)]
    largest = reach if full else min(reach, max(-(-total // count), total * weights[0] // sum(weights)))
    least = 1 if total - largest >= count - 1 else 0
    counts, surplus = [largest] + [least] * (count - 1), total - largest - least * (count - 1)
    while surplus > 0:
        candidates = [i for i in range(1, count) if counts[i] < largest] or [i for i in range(1, count) if counts[i] < reach]
        mass, remaining = sum([weights[i] for i in candidates]), surplus
        for i in candidates:
            addition = min(reach - counts[i], max(1, remaining * weights[i] // mass), surplus)
            counts[i] = counts[i] + addition
            surplus = surplus - addition
    return np.array(counts)


def normal_values(rng, shape, spread, bound, cuts=(), kind=jnp.bfloat16):
    loudness = block_levels(rng, shape, cuts, -0.22, 0.18) if cuts else 1.0
    drawn = jax.random.normal(rng, shape, jnp.float32) * spread * loudness
    return jnp.minimum(jnp.maximum(drawn, -bound), bound).astype(kind)


def setup_inputs(seed: int = 0, part: int = 0) -> dict:
    keys = jax.random.split(jax.random.key(seed), 8)
    own_keys = jax.random.split(jax.random.fold_in(keys[7], part), 8)
    tokens = normal_values(own_keys[0], (TOKENS, D), 1.0, 6.0, ((0, 16),))
    norm_gain = jnp.clip(1.0 + 0.18 * jax.random.normal(keys[1], (D,), jnp.float32), 0.1, 1.9)
    expert_ids_keys = jax.random.split(jax.random.fold_in(own_keys[2], 1), TOKENS // TOK_DEV)
    expert_ids_turns = jax.random.permutation(jax.random.fold_in(own_keys[2], 3), TOKENS // TOK_DEV)
    expert_ids = jax.vmap(lambda own, number: shared_out(jax.random.fold_in(own_keys[2], 2), own, number, TOK_DEV, EXPERTS, TOPK, CAP, 2))(expert_ids_keys, expert_ids_turns).reshape((TOKENS, TOPK))
    route_weights = jnp.clip(0.2 + 0.8 * jax.random.uniform(own_keys[3], (TOKENS, TOPK), jnp.float32) ** block_levels(own_keys[3], (TOKENS, TOPK), ((0, 16),), -0.2, 0.2), 0.2, 1.0)
    gate_proj = normal_values(keys[4], (EXPERTS, D, FF), (D // 9) ** -0.5, 0.375, ((0, 8), (2, 2)))
    linear_proj = normal_values(keys[5], (EXPERTS, D, FF), (D // 9) ** -0.5, 0.375, ((0, 8), (2, 2)))
    down_proj = normal_values(keys[6], (EXPERTS, FF, D), (FF * 64) ** -0.5, 0.01953125, ((0, 8), (1, 2)))
    return dict(tokens=tokens, norm_gain=norm_gain, expert_ids=expert_ids, route_weights=route_weights, gate_proj=gate_proj, linear_proj=linear_proj, down_proj=down_proj)


def expert_apply(rows, w_gate, w_lin, w_down):
    gate_pre = jnp.dot(rows, w_gate, preferred_element_type=jnp.float32)
    lin_pre = jnp.dot(rows, w_lin, preferred_element_type=jnp.float32)
    glu = jnp.minimum(gate_pre, 7.0)
    lin = jnp.clip(lin_pre, -7.0, 7.0)
    act = (glu * jax.nn.sigmoid(1.702 * glu) * (lin + 1.0)).astype(jnp.bfloat16)
    width = FF // N_TP
    total = jnp.zeros((rows.shape[0], D), jnp.float32)
    for block in range(N_TP):
        partial_value = jnp.dot(act[:, block * width:(block + 1) * width], w_down[block * width:(block + 1) * width], preferred_element_type=jnp.float32).astype(jnp.bfloat16)
        partial_value = lax.optimization_barrier(partial_value)
        total = total + partial_value.astype(jnp.float32)
    return total.astype(jnp.bfloat16)

def reference(tokens, norm_gain, expert_ids, route_weights, gate_proj, linear_proj, down_proj):
    values = tokens.astype(jnp.float32)
    normed = (values * lax.rsqrt(lax.optimization_barrier(jnp.mean(values * values, axis=-1, keepdims=True)) + 1e-06) * norm_gain).astype(jnp.bfloat16)
    flat = expert_ids.reshape(-1).astype(jnp.int32)
    onehot = (flat[:, None] == jnp.arange(EXPERTS, dtype=jnp.int32)[None, :]).astype(jnp.int32)
    slots = lax.optimization_barrier(jnp.sum((jnp.cumsum(onehot, axis=0) - 1) * onehot, axis=1)).astype(jnp.int32)
    per_expert = N_EP * N_TP * CAP
    where = (flat * per_expert + slots).astype(jnp.int32)
    buffer = jnp.zeros((EXPERTS * per_expert, D), jnp.bfloat16).at[where].set(jnp.repeat(normed, TOPK, axis=0))
    buffer = buffer.reshape(EXPERTS, per_expert, D)
    results = lax.map(lambda item: expert_apply(item[0], item[1], item[2], item[3]), (buffer, gate_proj, linear_proj, down_proj))
    picked = results.reshape(EXPERTS * per_expert, D)[where].reshape(TOKENS, TOPK, D).astype(jnp.float32)
    return lax.optimization_barrier(jnp.sum(picked * route_weights[:, :, None], axis=1)).astype(jnp.bfloat16)
```

```python
import functools

import jax
import jax.numpy as jnp
from jax import lax
from jax.experimental import pallas as pl
from jax.experimental.pallas import tpu as pltpu
from jax.sharding import PartitionSpec as P

MESH = pl.DeviceIdType.MESH


def shards(tokens, norm_gain, expert_ids, route_weights, gate_proj, linear_proj, down_proj):
    tok_count, width = tokens.shape
    picks = expert_ids.shape[1]
    experts = lax.axis_size("ep")
    capacity = 2 * tok_count * picks // experts
    values = tokens.astype(jnp.float32)
    normed = (
        values * lax.rsqrt(jnp.mean(values * values, axis=-1, keepdims=True) + 1e-06) * norm_gain
    ).astype(jnp.bfloat16)
    flat = expert_ids.reshape(-1)
    onehot = (flat[:, None] == jnp.arange(experts, dtype=jnp.int32)[None, :]).astype(jnp.int32)
    slots = jnp.sum((jnp.cumsum(onehot, axis=0) - 1) * onehot, axis=1)
    where = flat * capacity + slots
    buffer = (
        jnp.zeros((experts * capacity, width), jnp.bfloat16)
        .at[where]
        .set(jnp.repeat(normed, picks, axis=0))
    )
    arrived = lax.all_to_all(buffer, "ep", split_axis=0, concat_axis=0, tiled=True)
    rows = lax.all_gather(arrived, "tp", axis=0, tiled=True)
    gate_pre = jnp.dot(rows, gate_proj[0], preferred_element_type=jnp.float32)
    lin_pre = jnp.dot(rows, linear_proj[0], preferred_element_type=jnp.float32)
    glu = jnp.minimum(gate_pre, 7.0)
    lin = jnp.clip(lin_pre, -7.0, 7.0)
    hidden = (glu * jax.nn.sigmoid(1.702 * glu) * (lin + 1.0)).astype(jnp.bfloat16)
    rows = hidden
    summed = lax.psum_scatter(
        jnp.dot(rows, down_proj[0], preferred_element_type=jnp.float32).astype(jnp.bfloat16),
        "tp",
        scatter_dimension=0,
        tiled=True,
    )
    returned = lax.all_to_all(summed, "ep", split_axis=0, concat_axis=0, tiled=True)
    picked = returned[where].reshape(tok_count, picks, width).astype(jnp.float32)
    return jnp.sum(picked * route_weights[:, :, None], axis=1).astype(jnp.bfloat16)


def kernel(
    line, ids_ref, weights_ref, gain_ref, tokens_ref, gate_hbm, linear_hbm, down_hbm, out_ref,
    gate, linear, down, tok, meta, rows, cross, hidden, part, part_in, done, done_in, back, back_in,
    load_sem, tok_send, tok_recv, meta_send, meta_recv, cross_send, cross_recv, pair_send, pair_recv,
    part_send, part_recv, done_send, done_recv, back_send, back_recv,
):
    ep, core = lax.axis_index("ep"), lax.axis_index("tp")
    z, y = ep // 2, ep % 2
    experts = 2 * line
    tok_count, width = tokens_ref.shape
    capacity = rows.shape[3]
    ff = gate.shape[1]
    at_y = {"ep": z * 2 + 1 - y}
    at_core = {"tp": 1 - core}

    def at_z(other):
        return {"ep": other * 2 + y}

    def remote(source, target, send, recv, device):
        return pltpu.make_async_remote_copy(
            src_ref=source, dst_ref=target, send_sem=send, recv_sem=recv,
            device_id=device, device_id_type=MESH,
        )

    loads = [
        pltpu.make_async_copy(source, target, load_sem.at[i])
        for i, (source, target) in enumerate(((gate_hbm, gate), (linear_hbm, linear), (down_hbm, down)))
    ]
    for load in loads:
        load.start()
    barrier = pltpu.get_barrier_semaphore()
    for step in range(1, line):
        pl.semaphore_signal(barrier, 1, device_id=at_z((z + step) % line), device_id_type=MESH)
    pl.semaphore_signal(barrier, 1, device_id=at_y, device_id_type=MESH)
    pl.semaphore_signal(barrier, 1, device_id=at_core, device_id_type=MESH)

    def normalize(i, _):
        span = pl.ds(pl.multiple_of(i * 32, 32), 32)
        values = tokens_ref[span, :].astype(jnp.float32)
        scale = lax.rsqrt(jnp.mean(values * values, axis=-1, keepdims=True) + 1e-06)
        tok[z, span, :] = (values * scale * gain_ref[...]).astype(jnp.bfloat16)
        return 0

    lax.fori_loop(0, tok_count // 32, normalize, 0)
    names = lax.broadcasted_iota(jnp.int32, (experts, tok_count), 0)
    share = jnp.zeros((experts, tok_count), jnp.float32)
    chosen = jnp.zeros((experts, tok_count), jnp.float32)
    for pick in range(ids_ref.shape[0]):
        same = ids_ref[pick : pick + 1, :] == names
        share = share + jnp.where(same, weights_ref[pick : pick + 1, :], 0.0)
        chosen = chosen + jnp.where(same, 1.0, 0.0)
    first = lax.broadcasted_iota(jnp.int32, (tok_count, tok_count), 0)
    second = lax.broadcasted_iota(jnp.int32, (tok_count, tok_count), 1)
    eye = first == second
    before = jnp.where(first < second, 1.0, 0.0).astype(jnp.bfloat16)
    slots = jnp.dot(chosen.astype(jnp.bfloat16), before, preferred_element_type=jnp.float32)
    meta[z, 0:experts, :] = jnp.where(chosen > 0.5, slots, -1.0)
    meta[z, experts : 2 * experts, :] = share
    pl.semaphore_wait(barrier, line + 1)

    def meta_copy(step):
        return remote(meta.at[z], meta.at[z], meta_send.at[step], meta_recv.at[z], at_z((z + step) % line))

    def meta_arrival(source):
        return remote(meta.at[source], meta.at[source], meta_send.at[0], meta_recv.at[source], at_z((z + 1) % line))

    for step in range(1, line):
        meta_copy(step).start()

    def order(step):
        found = z
        for place in range(line):
            nearest = sorted(range(line), key=lambda other: (abs(other - place), other))
            found = jnp.where(z == place, nearest[step], found)
        return found if step else z

    def hop(source, side):
        return remote(
            tok.at[source], tok.at[source], tok_send.at[source, side], tok_recv.at[source],
            at_z(lax.rem(z + (1 if side else line - 1), line)),
        )

    def hops(source, act):
        @pl.when((source <= z) & (z < line - 1))
        def _():
            act(hop(source, 1))

        @pl.when((source >= z) & (z > 0))
        def _():
            act(hop(source, 0))

    def cross_copy(source):
        return remote(cross.at[source], rows.at[source, core, y], cross_send.at[source], cross_recv.at[source], at_y)

    def cross_arrival(source):
        return remote(cross.at[source], rows.at[source, core, 1 - y], cross_send.at[source], cross_recv.at[source], at_y)

    def pair_copy(source, column):
        block = rows.at[source, core, column]
        return remote(block, block, pair_send.at[source, column], pair_recv.at[source, column], at_core)

    def pair_arrival(source, column):
        block = rows.at[source, 1 - core, column]
        return remote(block, block, pair_send.at[source, column], pair_recv.at[source, column], at_core)

    def part_copy(source):
        return remote(part.at[source, 1 - core], part_in.at[source], part_send.at[source], part_recv.at[source], at_core)

    def done_copy(source):
        return remote(done.at[source, 1 - y], done_in.at[source], done_send.at[source], done_recv.at[source], at_y)

    def back_copy(source):
        return remote(back.at[source], back_in.at[z], back_send.at[source], back_recv.at[z], at_z(source))

    def back_arrival(source):
        return remote(back.at[source], back_in.at[source], back_send.at[source], back_recv.at[source], at_z(source))

    tile = 512

    def over_width(act):
        def go(i, _):
            act(pl.ds(pl.multiple_of(i * tile, tile), tile))
            return 0

        lax.fori_loop(0, width // tile, go, 0)

    def dispatch(step):
        source = order(step)
        if step:
            hop(source, 0).wait_recv()
        hops(source, lambda copy: copy.start())
        if step:
            meta_arrival(source).wait_recv()
        place = lax.broadcasted_iota(jnp.int32, (capacity, tok_count), 0).astype(jnp.float32)
        away = (meta[source, pl.ds(z * 2 + 1 - y, 1), :] == place).astype(jnp.bfloat16)
        here = (meta[source, pl.ds(z * 2 + y, 1), :] == place).astype(jnp.bfloat16)

        def send_away(span):
            cross[source, :, span] = jnp.dot(
                away, tok[source, :, span], preferred_element_type=jnp.float32
            ).astype(jnp.bfloat16)

        def keep_here(span):
            rows[source, core, y, :, span] = jnp.dot(
                here, tok[source, :, span], preferred_element_type=jnp.float32
            ).astype(jnp.bfloat16)

        over_width(send_away)
        cross_copy(source).start()
        over_width(keep_here)
        pair_copy(source, y).start()

    def forward(step):
        source = order(step)
        cross_arrival(source).wait_recv()
        pair_copy(source, 1 - y).start()

    def compute(step):
        source = order(step)
        for column in range(2):
            pair_arrival(source, column).wait_recv()
        if step == 0:
            loads[0].wait()
            loads[1].wait()
        depth = 256

        def up(i, _):
            span = pl.ds(pl.multiple_of(i * depth, depth), depth)
            block = rows[source].reshape(4 * capacity, width)
            glu = jnp.minimum(jnp.dot(block, gate[:, span], preferred_element_type=jnp.float32), 7.0)
            lin = jnp.clip(jnp.dot(block, linear[:, span], preferred_element_type=jnp.float32), -7.0, 7.0)
            hidden[:, span] = (glu * jax.nn.sigmoid(1.702 * glu) * (lin + 1.0)).astype(jnp.bfloat16)
            return 0

        lax.fori_loop(0, ff // depth, up, 0)
        if step == 0:
            loads[2].wait()

        def out(span):
            part[source, :, :, :, span] = (
                jnp.dot(hidden[...], down[:, span], preferred_element_type=jnp.float32)
                .astype(jnp.bfloat16)
                .reshape(2, 2, capacity, tile)
            )

        over_width(out)
        part_copy(source).start()

    def finish(step):
        source = order(step)
        part_copy(source).wait_recv()

        def add(span):
            total = part[source, core, :, :, span].astype(jnp.float32) + part_in[source, :, :, span].astype(
                jnp.float32
            )
            done[source, :, :, span] = total.astype(jnp.bfloat16)

        over_width(add)
        done_copy(source).start()

    def combine(step):
        source = order(step)
        done_copy(source).wait_recv()
        lane = lax.broadcasted_iota(jnp.int32, (tok_count, capacity), 1).astype(jnp.float32)

        def column(row):
            return jnp.sum(jnp.where(eye, meta[source, pl.ds(row, 1), :], 0.0), axis=1, keepdims=True)

        mine, other = z * 2 + y, z * 2 + 1 - y
        spread_mine = (column(mine) == lane).astype(jnp.bfloat16)
        spread_other = (column(other) == lane).astype(jnp.bfloat16)
        share_mine, share_other = column(experts + mine), column(experts + other)

        def merge(span):
            total = share_mine * jnp.dot(
                spread_mine, done[source, y, :, span], preferred_element_type=jnp.float32
            ) + share_other * jnp.dot(spread_other, done_in[source, :, span], preferred_element_type=jnp.float32)
            back[source, :, span] = total.astype(jnp.bfloat16)

        over_width(merge)
        if step:
            back_copy(source).start()

    for tick in range(line + 2):
        if tick < line:
            dispatch(tick)
        if 0 <= tick - 1 < line:
            compute(tick - 1)
        if tick < line:
            forward(tick)
        if 0 <= tick - 1 < line:
            finish(tick - 1)
        if 0 <= tick - 2 < line:
            combine(tick - 2)
    for step in range(1, line):
        back_arrival(order(step)).wait_recv()

    def gather(span):
        total = back[z, :, span].astype(jnp.float32)
        for step in range(1, line):
            total = total + back_in[order(step), :, span].astype(jnp.float32)
        out_ref[:, span] = total.astype(jnp.bfloat16)

    over_width(gather)
    for step in range(line):
        source = order(step)
        hops(source, lambda copy: copy.wait_send())
        if step:
            meta_copy(step).wait_send()
            back_copy(source).wait_send()
        cross_copy(source).wait_send()
        for column in range(2):
            pair_copy(source, column).wait_send()
        part_copy(source).wait_send()
        done_copy(source).wait_send()


def fused(line, tokens, norm_gain, expert_ids, route_weights, gate_proj, linear_proj, down_proj):
    tok_count, width = tokens.shape
    picks = expert_ids.shape[1]
    experts = 2 * line
    capacity = 2 * tok_count * picks // experts
    ff = gate_proj.shape[2]
    wide, dma = jnp.bfloat16, pltpu.SemaphoreType.DMA
    inside, outside = pl.BlockSpec(memory_space=pltpu.VMEM), pl.BlockSpec(memory_space=pl.ANY)
    return pl.pallas_call(
        functools.partial(kernel, line),
        out_shape=jax.ShapeDtypeStruct((tok_count, width), wide),
        in_specs=[inside] * 4 + [outside] * 3,
        out_specs=inside,
        scratch_shapes=[
            pltpu.VMEM((width, ff), wide),
            pltpu.VMEM((width, ff), wide),
            pltpu.VMEM((ff, width), wide),
            pltpu.VMEM((line, tok_count, width), wide),
            pltpu.VMEM((line, 2 * experts, tok_count), jnp.float32),
            pltpu.VMEM((line, 2, 2, capacity, width), wide),
            pltpu.VMEM((line, capacity, width), wide),
            pltpu.VMEM((4 * capacity, ff), wide),
            pltpu.VMEM((line, 2, 2, capacity, width), wide),
            pltpu.VMEM((line, 2, capacity, width), wide),
            pltpu.VMEM((line, 2, capacity, width), wide),
            pltpu.VMEM((line, capacity, width), wide),
            pltpu.VMEM((line, tok_count, width), wide),
            pltpu.VMEM((line, tok_count, width), wide),
            dma((3,)),
            dma((line, 2)), dma((line,)),
            dma((line,)), dma((line,)),
            dma((line,)), dma((line,)),
            dma((line, 2)), dma((line, 2)),
            dma((line,)), dma((line,)),
            dma((line,)), dma((line,)),
            dma((line,)), dma((line,)),
        ],
        compiler_params=pltpu.CompilerParams(
            collective_id=0, has_side_effects=True, vmem_limit_bytes=60 * 1024 * 1024
        ),
        name="experts",
    )(
        expert_ids.T, route_weights.T, norm_gain.reshape(1, width), tokens,
        gate_proj[0], linear_proj[0], down_proj[0],
    )


def solution(mesh):
    placed = (
        P(("grp", "ep", "tp"), None),
        P(),
        P(("grp", "ep", "tp"), None),
        P(("grp", "ep", "tp"), None),
        P("ep", None, "tp"),
        P("ep", None, "tp"),
        P("ep", "tp", None),
    )
    along = [device.coords[2] for device in mesh.devices[0, :, 0]]
    line = len(set(along))
    paired = line > 1 and along == [index // 2 for index in range(2 * line)] and mesh.shape["tp"] == 2
    return jax.shard_map(
        functools.partial(fused, line) if paired else shards,
        mesh=mesh,
        in_specs=placed,
        out_specs=P(("grp", "ep", "tp"), None),
        check_vma=False,
    )
```

```python
import functools

import jax
import jax.numpy as jnp
from jax import lax
from jax.experimental import pallas as pl
from jax.experimental.pallas import tpu as pltpu
from jax.sharding import PartitionSpec as P

MESH = pl.DeviceIdType.MESH
PARTS = 2


def shards(tokens, norm_gain, expert_ids, route_weights, gate_proj, linear_proj, down_proj):
    tok_count, width = tokens.shape
    picks = expert_ids.shape[1]
    experts = lax.axis_size("ep")
    capacity = 2 * tok_count * picks // experts
    values = tokens.astype(jnp.float32)
    normed = (
        values * lax.rsqrt(jnp.mean(values * values, axis=-1, keepdims=True) + 1e-06) * norm_gain
    ).astype(jnp.bfloat16)
    flat = expert_ids.reshape(-1)
    onehot = (flat[:, None] == jnp.arange(experts, dtype=jnp.int32)[None, :]).astype(jnp.int32)
    slots = jnp.sum((jnp.cumsum(onehot, axis=0) - 1) * onehot, axis=1)
    where = flat * capacity + slots
    buffer = (
        jnp.zeros((experts * capacity, width), jnp.bfloat16)
        .at[where]
        .set(jnp.repeat(normed, picks, axis=0))
    )
    arrived = lax.all_to_all(buffer, "ep", split_axis=0, concat_axis=0, tiled=True)
    rows = lax.all_gather(arrived, "tp", axis=0, tiled=True)
    gate_pre = jnp.dot(rows, gate_proj[0], preferred_element_type=jnp.float32)
    lin_pre = jnp.dot(rows, linear_proj[0], preferred_element_type=jnp.float32)
    glu = jnp.minimum(gate_pre, 7.0)
    lin = jnp.clip(lin_pre, -7.0, 7.0)
    hidden = (glu * jax.nn.sigmoid(1.702 * glu) * (lin + 1.0)).astype(jnp.bfloat16)
    rows = hidden
    summed = lax.psum_scatter(
        jnp.dot(rows, down_proj[0], preferred_element_type=jnp.float32).astype(jnp.bfloat16),
        "tp",
        scatter_dimension=0,
        tiled=True,
    )
    returned = lax.all_to_all(summed, "ep", split_axis=0, concat_axis=0, tiled=True)
    picked = returned[where].reshape(tok_count, picks, width).astype(jnp.float32)
    return jnp.sum(picked * route_weights[:, :, None], axis=1).astype(jnp.bfloat16)


def kernel(
    line, ids_ref, weights_ref, gain_ref, tokens_ref, gate_hbm, linear_hbm, down_hbm, out_ref,
    gate, linear, down, tok, meta, rows, cross, hidden, part, part_in, done, done_in, back, back_in,
    load_sem, tok_send, tok_recv, meta_send, meta_recv, cross_send, cross_recv, pair_send, pair_recv,
    part_send, part_recv, done_send, done_recv, back_send, back_recv,
):
    ep, core = lax.axis_index("ep"), lax.axis_index("tp")
    z, y = ep // 2, ep % 2
    experts = 2 * line
    tok_count, width = tokens_ref.shape
    capacity = rows.shape[3]
    ff = gate.shape[1]
    half = width // PARTS
    cols = [slice(i * half, (i + 1) * half) for i in range(PARTS)]
    at_y = {"ep": z * 2 + 1 - y}
    at_core = {"tp": 1 - core}

    def at_z(other):
        return {"ep": other * 2 + y}

    def remote(source, target, send, recv, device):
        return pltpu.make_async_remote_copy(
            src_ref=source, dst_ref=target, send_sem=send, recv_sem=recv,
            device_id=device, device_id_type=MESH,
        )

    loads = [
        pltpu.make_async_copy(source, target, load_sem.at[i])
        for i, (source, target) in enumerate(((gate_hbm, gate), (linear_hbm, linear), (down_hbm, down)))
    ]
    for load in loads:
        load.start()
    barrier = pltpu.get_barrier_semaphore()
    for step in range(1, line):
        pl.semaphore_signal(barrier, 1, device_id=at_z((z + step) % line), device_id_type=MESH)
    pl.semaphore_signal(barrier, 1, device_id=at_y, device_id_type=MESH)
    pl.semaphore_signal(barrier, 1, device_id=at_core, device_id_type=MESH)

    def normalize(i, _):
        span = pl.ds(pl.multiple_of(i * 32, 32), 32)
        values = tokens_ref[span, :].astype(jnp.float32)
        scale = lax.rsqrt(jnp.mean(values * values, axis=-1, keepdims=True) + 1e-06)
        tok[z, span, :] = (values * scale * gain_ref[...]).astype(jnp.bfloat16)
        return 0

    lax.fori_loop(0, tok_count // 32, normalize, 0)
    names = lax.broadcasted_iota(jnp.int32, (experts, tok_count), 0)
    share = jnp.zeros((experts, tok_count), jnp.float32)
    chosen = jnp.zeros((experts, tok_count), jnp.float32)
    for pick in range(ids_ref.shape[0]):
        same = ids_ref[pick : pick + 1, :] == names
        share = share + jnp.where(same, weights_ref[pick : pick + 1, :], 0.0)
        chosen = chosen + jnp.where(same, 1.0, 0.0)
    first = lax.broadcasted_iota(jnp.int32, (tok_count, tok_count), 0)
    second = lax.broadcasted_iota(jnp.int32, (tok_count, tok_count), 1)
    eye = first == second
    before = jnp.where(first < second, 1.0, 0.0).astype(jnp.bfloat16)
    slots = jnp.dot(chosen.astype(jnp.bfloat16), before, preferred_element_type=jnp.float32)
    meta[z, 0:experts, :] = jnp.where(chosen > 0.5, slots, -1.0)
    meta[z, experts : 2 * experts, :] = share
    pl.semaphore_wait(barrier, line + 1)

    def meta_copy(step):
        return remote(meta.at[z], meta.at[z], meta_send.at[step], meta_recv.at[z], at_z((z + step) % line))

    def meta_arrival(source):
        return remote(meta.at[source], meta.at[source], meta_send.at[0], meta_recv.at[source], at_z((z + 1) % line))

    for step in range(1, line):
        meta_copy(step).start()

    def order(step):
        found = z
        for place in range(line):
            nearest = sorted(range(line), key=lambda other: (abs(other - place), other))
            found = jnp.where(z == place, nearest[step], found)
        return found if step else z

    def hop(source, i, side):
        block = tok.at[source, :, cols[i]]
        return remote(
            block, block, tok_send.at[source, i, side], tok_recv.at[source, i],
            at_z(lax.rem(z + (1 if side else line - 1), line)),
        )

    def hops(source, i, act):
        @pl.when((source <= z) & (z < line - 1))
        def _():
            act(hop(source, i, 1))

        @pl.when((source >= z) & (z > 0))
        def _():
            act(hop(source, i, 0))

    def cross_copy(source, i):
        return remote(
            cross.at[source, :, cols[i]], rows.at[source, core, y, :, cols[i]],
            cross_send.at[source, i], cross_recv.at[source, i], at_y,
        )

    def cross_arrival(source, i):
        return remote(
            cross.at[source, :, cols[i]], rows.at[source, core, 1 - y, :, cols[i]],
            cross_send.at[source, i], cross_recv.at[source, i], at_y,
        )

    def pair_move(source, owner, column, i):
        block = rows.at[source, owner, column, :, cols[i]]
        return remote(block, block, pair_send.at[source, column, i], pair_recv.at[source, column, i], at_core)

    def part_copy(source, i):
        return remote(
            part.at[source, 1 - core, :, :, cols[i]], part_in.at[source, :, :, cols[i]],
            part_send.at[source, i], part_recv.at[source, i], at_core,
        )

    def done_copy(source, i):
        return remote(
            done.at[source, 1 - y, :, cols[i]], done_in.at[source, :, cols[i]],
            done_send.at[source, i], done_recv.at[source, i], at_y,
        )

    def back_copy(source, i):
        return remote(
            back.at[source, :, cols[i]], back_in.at[z, :, cols[i]],
            back_send.at[source, i], back_recv.at[z, i], at_z(source),
        )

    def back_arrival(source, i):
        return remote(
            back.at[source, :, cols[i]], back_in.at[source, :, cols[i]],
            back_send.at[source, i], back_recv.at[source, i], at_z(source),
        )

    tile = 512

    def over_width(i, act):
        def go(j, _):
            act(pl.ds(pl.multiple_of(i * half + j * tile, tile), tile))
            return 0

        lax.fori_loop(0, half // tile, go, 0)

    def arrive(tick, i):
        if tick == 0:
            hops(z, i, lambda copy: copy.start())
        for step in range(max(tick, 1), line):
            source = order(step)
            apart = jnp.where(source > z, source - z, z - source)

            @pl.when(apart == tick)
            def _():
                hop(source, i, 0).wait_recv()
                hops(source, i, lambda copy: copy.start())

    def dispatch(step):
        source = order(step)
        place = lax.broadcasted_iota(jnp.int32, (capacity, tok_count), 0).astype(jnp.float32)
        if step:
            meta_arrival(source).wait_recv()
        away = (meta[source, pl.ds(z * 2 + 1 - y, 1), :] == place).astype(jnp.bfloat16)
        here = (meta[source, pl.ds(z * 2 + y, 1), :] == place).astype(jnp.bfloat16)

        def send_away(span):
            cross[source, :, span] = jnp.dot(
                away, tok[source, :, span], preferred_element_type=jnp.float32
            ).astype(jnp.bfloat16)

        def keep_here(span):
            rows[source, core, y, :, span] = jnp.dot(
                here, tok[source, :, span], preferred_element_type=jnp.float32
            ).astype(jnp.bfloat16)

        if step == 0:
            for i in range(PARTS):
                arrive(step, i)
        for i in range(PARTS):
            if step:
                arrive(step, i)
            over_width(i, send_away)
            cross_copy(source, i).start()
            over_width(i, keep_here)
            pair_move(source, core, y, i).start()

    def forward(step):
        source = order(step)
        for i in range(PARTS):
            cross_arrival(source, i).wait_recv()
            pair_move(source, core, 1 - y, i).start()

    def compute(step):
        source = order(step)
        for column in range(2):
            for i in range(PARTS):
                pair_move(source, 1 - core, column, i).wait_recv()
        if step == 0:
            loads[0].wait()
            loads[1].wait()
        depth = 256

        def up(i, _):
            span = pl.ds(pl.multiple_of(i * depth, depth), depth)
            block = rows[source].reshape(4 * capacity, width)
            glu = jnp.minimum(jnp.dot(block, gate[:, span], preferred_element_type=jnp.float32), 7.0)
            lin = jnp.clip(jnp.dot(block, linear[:, span], preferred_element_type=jnp.float32), -7.0, 7.0)
            hidden[:, span] = (glu * jax.nn.sigmoid(1.702 * glu) * (lin + 1.0)).astype(jnp.bfloat16)
            return 0

        lax.fori_loop(0, ff // depth, up, 0)
        if step == 0:
            loads[2].wait()

        def out(span):
            part[source, :, :, :, span] = (
                jnp.dot(hidden[...], down[:, span], preferred_element_type=jnp.float32)
                .astype(jnp.bfloat16)
                .reshape(2, 2, capacity, tile)
            )

        for i in range(PARTS):
            over_width(i, out)
            part_copy(source, i).start()

    def finish(step):
        source = order(step)

        def add(span):
            total = part[source, core, :, :, span].astype(jnp.float32) + part_in[source, :, :, span].astype(
                jnp.float32
            )
            done[source, :, :, span] = total.astype(jnp.bfloat16)

        for i in range(PARTS):
            part_copy(source, i).wait_recv()
            over_width(i, add)
            done_copy(source, i).start()

    def combine(step):
        source = order(step)
        lane = lax.broadcasted_iota(jnp.int32, (tok_count, capacity), 1).astype(jnp.float32)

        def column(row):
            return jnp.sum(jnp.where(eye, meta[source, pl.ds(row, 1), :], 0.0), axis=1, keepdims=True)

        mine, other = z * 2 + y, z * 2 + 1 - y
        spread_mine = (column(mine) == lane).astype(jnp.bfloat16)
        spread_other = (column(other) == lane).astype(jnp.bfloat16)
        share_mine, share_other = column(experts + mine), column(experts + other)

        def merge(span):
            total = share_mine * jnp.dot(
                spread_mine, done[source, y, :, span], preferred_element_type=jnp.float32
            ) + share_other * jnp.dot(spread_other, done_in[source, :, span], preferred_element_type=jnp.float32)
            back[source, :, span] = total.astype(jnp.bfloat16)

        for i in range(PARTS):
            done_copy(source, i).wait_recv()
            over_width(i, merge)
            if step:
                back_copy(source, i).start()

    for tick in range(line + 2):
        if tick < line:
            dispatch(tick)
        if 0 <= tick - 1 < line:
            compute(tick - 1)
        if tick == line:
            finish(tick - 1)
        if 0 <= tick - 2 < line:
            combine(tick - 2)
        if tick < line:
            forward(tick)
        if 0 <= tick - 1 < line - 1:
            finish(tick - 1)

    def gather(span):
        total = back[z, :, span].astype(jnp.float32)
        for step in range(1, line):
            total = total + back_in[order(step), :, span].astype(jnp.float32)
        out_ref[:, span] = total.astype(jnp.bfloat16)

    for i in range(PARTS):
        for step in range(1, line):
            back_arrival(order(step), i).wait_recv()
        over_width(i, gather)
    for step in range(line):
        source = order(step)
        if step:
            meta_copy(step).wait_send()
        for i in range(PARTS):
            hops(source, i, lambda copy: copy.wait_send())
            if step:
                back_copy(source, i).wait_send()
            cross_copy(source, i).wait_send()
            for column in range(2):
                pair_move(source, core, column, i).wait_send()
            part_copy(source, i).wait_send()
            done_copy(source, i).wait_send()


def fused(line, tokens, norm_gain, expert_ids, route_weights, gate_proj, linear_proj, down_proj):
    tok_count, width = tokens.shape
    picks = expert_ids.shape[1]
    experts = 2 * line
    capacity = 2 * tok_count * picks // experts
    ff = gate_proj.shape[2]
    wide, dma = jnp.bfloat16, pltpu.SemaphoreType.DMA
    inside, outside = pl.BlockSpec(memory_space=pltpu.VMEM), pl.BlockSpec(memory_space=pl.ANY)
    return pl.pallas_call(
        functools.partial(kernel, line),
        out_shape=jax.ShapeDtypeStruct((tok_count, width), wide),
        in_specs=[inside] * 4 + [outside] * 3,
        out_specs=inside,
        scratch_shapes=[
            pltpu.VMEM((width, ff), wide),
            pltpu.VMEM((width, ff), wide),
            pltpu.VMEM((ff, width), wide),
            pltpu.VMEM((line, tok_count, width), wide),
            pltpu.VMEM((line, 2 * experts, tok_count), jnp.float32),
            pltpu.VMEM((line, 2, 2, capacity, width), wide),
            pltpu.VMEM((line, capacity, width), wide),
            pltpu.VMEM((4 * capacity, ff), wide),
            pltpu.VMEM((line, 2, 2, capacity, width), wide),
            pltpu.VMEM((line, 2, capacity, width), wide),
            pltpu.VMEM((line, 2, capacity, width), wide),
            pltpu.VMEM((line, capacity, width), wide),
            pltpu.VMEM((line, tok_count, width), wide),
            pltpu.VMEM((line, tok_count, width), wide),
            dma((3,)),
            dma((line, PARTS, 2)), dma((line, PARTS)),
            dma((line,)), dma((line,)),
            dma((line, PARTS)), dma((line, PARTS)),
            dma((line, 2, PARTS)), dma((line, 2, PARTS)),
            dma((line, PARTS)), dma((line, PARTS)),
            dma((line, PARTS)), dma((line, PARTS)),
            dma((line, PARTS)), dma((line, PARTS)),
        ],
        compiler_params=pltpu.CompilerParams(
            collective_id=0, has_side_effects=True, vmem_limit_bytes=60 * 1024 * 1024
        ),
        name="experts",
    )(
        expert_ids.T, route_weights.T, norm_gain.reshape(1, width), tokens,
        gate_proj[0], linear_proj[0], down_proj[0],
    )


def solution(mesh):
    placed = (
        P(("grp", "ep", "tp"), None),
        P(),
        P(("grp", "ep", "tp"), None),
        P(("grp", "ep", "tp"), None),
        P("ep", None, "tp"),
        P("ep", None, "tp"),
        P("ep", "tp", None),
    )
    along = [device.coords[2] for device in mesh.devices[0, :, 0]]
    line = len(set(along))
    paired = line > 1 and along == [index // 2 for index in range(2 * line)] and mesh.shape["tp"] == 2
    return jax.shard_map(
        functools.partial(fused, line) if paired else shards,
        mesh=mesh,
        in_specs=placed,
        out_specs=P(("grp", "ep", "tp"), None),
        check_vma=False,
    )
```

```python
import functools

import jax
import jax.numpy as jnp
from jax import lax
from jax.experimental import pallas as pl
from jax.experimental.pallas import tpu as pltpu
from jax.sharding import PartitionSpec as P

MESH = pl.DeviceIdType.MESH
PARTS = 2


def shards(tokens, norm_gain, expert_ids, route_weights, gate_proj, linear_proj, down_proj):
    tok_count, width = tokens.shape
    picks = expert_ids.shape[1]
    experts = lax.axis_size("ep")
    capacity = 2 * tok_count * picks // experts
    values = tokens.astype(jnp.float32)
    normed = (
        values * lax.rsqrt(jnp.mean(values * values, axis=-1, keepdims=True) + 1e-06) * norm_gain
    ).astype(jnp.bfloat16)
    flat = expert_ids.reshape(-1)
    onehot = (flat[:, None] == jnp.arange(experts, dtype=jnp.int32)[None, :]).astype(jnp.int32)
    slots = jnp.sum((jnp.cumsum(onehot, axis=0) - 1) * onehot, axis=1)
    where = flat * capacity + slots
    buffer = (
        jnp.zeros((experts * capacity, width), jnp.bfloat16)
        .at[where]
        .set(jnp.repeat(normed, picks, axis=0))
    )
    arrived = lax.all_to_all(buffer, "ep", split_axis=0, concat_axis=0, tiled=True)
    rows = lax.all_gather(arrived, "tp", axis=0, tiled=True)
    gate_pre = jnp.dot(rows, gate_proj[0], preferred_element_type=jnp.float32)
    lin_pre = jnp.dot(rows, linear_proj[0], preferred_element_type=jnp.float32)
    glu = jnp.minimum(gate_pre, 7.0)
    lin = jnp.clip(lin_pre, -7.0, 7.0)
    hidden = (glu * jax.nn.sigmoid(1.702 * glu) * (lin + 1.0)).astype(jnp.bfloat16)
    rows = hidden
    summed = lax.psum_scatter(
        jnp.dot(rows, down_proj[0], preferred_element_type=jnp.float32).astype(jnp.bfloat16),
        "tp",
        scatter_dimension=0,
        tiled=True,
    )
    returned = lax.all_to_all(summed, "ep", split_axis=0, concat_axis=0, tiled=True)
    picked = returned[where].reshape(tok_count, picks, width).astype(jnp.float32)
    return jnp.sum(picked * route_weights[:, :, None], axis=1).astype(jnp.bfloat16)


def kernel(
    line, ids_ref, weights_ref, gain_ref, tokens_ref, gate_hbm, linear_hbm, down_hbm, out_ref,
    gate, linear, down, tok, meta, rows, cross, hidden, part, part_in, done, back_in, total,
    load_sem, tok_send, tok_recv, meta_send, meta_recv, cross_send, cross_recv, pair_send, pair_recv,
    part_send, part_recv, back_send, back_recv,
):
    ep, core = lax.axis_index("ep"), lax.axis_index("tp")
    z, y = ep // 2, ep % 2
    experts = 2 * line
    tok_count, width = tokens_ref.shape
    capacity = rows.shape[3]
    ff = gate.shape[1]
    half = width // PARTS
    cols = [slice(i * half, (i + 1) * half) for i in range(PARTS)]
    at_y = {"ep": z * 2 + 1 - y}
    at_core = {"tp": 1 - core}

    def at_z(other):
        return {"ep": other * 2 + y}

    def remote(source, target, send, recv, device):
        return pltpu.make_async_remote_copy(
            src_ref=source, dst_ref=target, send_sem=send, recv_sem=recv,
            device_id=device, device_id_type=MESH,
        )

    loads = [
        pltpu.make_async_copy(source, target, load_sem.at[i])
        for i, (source, target) in enumerate(((gate_hbm, gate), (linear_hbm, linear), (down_hbm, down)))
    ]
    for load in loads:
        load.start()
    barrier = pltpu.get_barrier_semaphore()
    for step in range(1, experts):
        pl.semaphore_signal(barrier, 1, device_id={"ep": (ep + step) % experts}, device_id_type=MESH)
    pl.semaphore_signal(barrier, 1, device_id=at_core, device_id_type=MESH)

    def normalize(i, _):
        span = pl.ds(pl.multiple_of(i * 32, 32), 32)
        values = tokens_ref[span, :].astype(jnp.float32)
        scale = lax.rsqrt(jnp.mean(values * values, axis=-1, keepdims=True) + 1e-06)
        tok[z, span, :] = (values * scale * gain_ref[...]).astype(jnp.bfloat16)
        return 0

    lax.fori_loop(0, tok_count // 32, normalize, 0)
    names = lax.broadcasted_iota(jnp.int32, (experts, tok_count), 0)
    share = jnp.zeros((experts, tok_count), jnp.float32)
    chosen = jnp.zeros((experts, tok_count), jnp.float32)
    for pick in range(ids_ref.shape[0]):
        same = ids_ref[pick : pick + 1, :] == names
        share = share + jnp.where(same, weights_ref[pick : pick + 1, :], 0.0)
        chosen = chosen + jnp.where(same, 1.0, 0.0)
    first = lax.broadcasted_iota(jnp.int32, (tok_count, tok_count), 0)
    second = lax.broadcasted_iota(jnp.int32, (tok_count, tok_count), 1)
    eye = first == second
    before = jnp.where(first < second, 1.0, 0.0).astype(jnp.bfloat16)
    slots = jnp.dot(chosen.astype(jnp.bfloat16), before, preferred_element_type=jnp.float32)
    meta[z, 0:experts, :] = jnp.where(chosen > 0.5, slots, -1.0)
    meta[z, experts : 2 * experts, :] = share
    pl.semaphore_wait(barrier, experts)

    def meta_copy(step):
        return remote(meta.at[z], meta.at[z], meta_send.at[step], meta_recv.at[z], at_z((z + step) % line))

    def meta_arrival(source):
        return remote(meta.at[source], meta.at[source], meta_send.at[0], meta_recv.at[source], at_z((z + 1) % line))

    for step in range(1, line):
        meta_copy(step).start()

    def order(step):
        found = z
        for place in range(line):
            nearest = sorted(range(line), key=lambda other: (abs(other - place), other))
            found = jnp.where(z == place, nearest[step], found)
        return found if step else z

    def hop(source, i, side):
        block = tok.at[source, :, cols[i]]
        return remote(
            block, block, tok_send.at[source, i, side], tok_recv.at[source, i],
            at_z(lax.rem(z + (1 if side else line - 1), line)),
        )

    def hops(source, i, act):
        @pl.when((source <= z) & (z < line - 1))
        def _():
            act(hop(source, i, 1))

        @pl.when((source >= z) & (z > 0))
        def _():
            act(hop(source, i, 0))

    def cross_copy(source, i):
        return remote(
            cross.at[source, :, cols[i]], rows.at[source, core, y, :, cols[i]],
            cross_send.at[source, i], cross_recv.at[source, i], at_y,
        )

    def cross_arrival(source, i):
        return remote(
            cross.at[source, :, cols[i]], rows.at[source, core, 1 - y, :, cols[i]],
            cross_send.at[source, i], cross_recv.at[source, i], at_y,
        )

    def pair_move(source, owner, column, i):
        block = rows.at[source, owner, column, :, cols[i]]
        return remote(block, block, pair_send.at[source, column, i], pair_recv.at[source, column, i], at_core)

    def part_copy(source, i):
        return remote(
            part.at[source, 1 - core, :, :, cols[i]], part_in.at[source, :, :, cols[i]],
            part_send.at[source, i], part_recv.at[source, i], at_core,
        )

    def back_copy(source, column, i):
        return remote(
            done.at[source, column, :, cols[i]], back_in.at[z, y, :, cols[i]],
            back_send.at[source, column, i], back_recv.at[z, y, i], {"ep": source * 2 + column},
        )

    def back_arrival(source, column, i):
        return remote(
            done.at[source, column, :, cols[i]], back_in.at[source, column, :, cols[i]],
            back_send.at[source, column, i], back_recv.at[source, column, i], {"ep": source * 2 + column},
        )

    tile = 512

    def over_width(i, act):
        def go(j, _):
            act(pl.ds(pl.multiple_of(i * half + j * tile, tile), tile))
            return 0

        lax.fori_loop(0, half // tile, go, 0)

    def arrive(tick, i):
        if tick == 0:
            hops(z, i, lambda copy: copy.start())
        for step in range(max(tick, 1), line):
            source = order(step)
            apart = jnp.where(source > z, source - z, z - source)

            @pl.when(apart == tick)
            def _():
                hop(source, i, 0).wait_recv()
                hops(source, i, lambda copy: copy.start())

    def dispatch(step):
        source = order(step)
        place = lax.broadcasted_iota(jnp.int32, (capacity, tok_count), 0).astype(jnp.float32)
        if step:
            meta_arrival(source).wait_recv()
        away = (meta[source, pl.ds(z * 2 + 1 - y, 1), :] == place).astype(jnp.bfloat16)
        here = (meta[source, pl.ds(z * 2 + y, 1), :] == place).astype(jnp.bfloat16)

        def send_away(span):
            cross[source, :, span] = jnp.dot(
                away, tok[source, :, span], preferred_element_type=jnp.float32
            ).astype(jnp.bfloat16)

        def keep_here(span):
            rows[source, core, y, :, span] = jnp.dot(
                here, tok[source, :, span], preferred_element_type=jnp.float32
            ).astype(jnp.bfloat16)

        if step == 0:
            for i in range(PARTS):
                arrive(step, i)
        for i in range(PARTS):
            if step:
                arrive(step, i)
            over_width(i, send_away)
            cross_copy(source, i).start()
            over_width(i, keep_here)
            pair_move(source, core, y, i).start()

    def forward(step):
        source = order(step)
        for i in range(PARTS):
            cross_arrival(source, i).wait_recv()
            pair_move(source, core, 1 - y, i).start()

    def compute(step):
        source = order(step)
        for column in range(2):
            for i in range(PARTS):
                pair_move(source, 1 - core, column, i).wait_recv()
        if step == 0:
            loads[0].wait()
            loads[1].wait()
        depth = 256

        def up(i, _):
            span = pl.ds(pl.multiple_of(i * depth, depth), depth)
            block = rows[source].reshape(4 * capacity, width)
            glu = jnp.minimum(jnp.dot(block, gate[:, span], preferred_element_type=jnp.float32), 7.0)
            lin = jnp.clip(jnp.dot(block, linear[:, span], preferred_element_type=jnp.float32), -7.0, 7.0)
            hidden[:, span] = (glu * jax.nn.sigmoid(1.702 * glu) * (lin + 1.0)).astype(jnp.bfloat16)
            return 0

        lax.fori_loop(0, ff // depth, up, 0)
        if step == 0:
            loads[2].wait()

        def out(span):
            part[source, :, :, :, span] = (
                jnp.dot(hidden[...], down[:, span], preferred_element_type=jnp.float32)
                .astype(jnp.bfloat16)
                .reshape(2, 2, capacity, tile)
            )

        for i in range(PARTS):
            over_width(i, out)
            part_copy(source, i).start()

    def finish(step):
        source = order(step)

        def add(span):
            whole = part[source, core, :, :, span].astype(jnp.float32) + part_in[source, :, :, span].astype(
                jnp.float32
            )
            done[source, :, :, span] = whole.astype(jnp.bfloat16)

        for i in range(PARTS):
            part_copy(source, i).wait_recv()
            over_width(i, add)
            back_copy(source, 1 - y, i).start()
            if step:
                back_copy(source, y, i).start()

    def gather(step, other):
        source, column = order(step), 1 - y if other else y
        expert = source * 2 + column
        lane = lax.broadcasted_iota(jnp.int32, (tok_count, capacity), 1).astype(jnp.float32)

        def upright(row):
            return jnp.sum(jnp.where(eye, meta[z, pl.ds(row, 1), :], 0.0), axis=1, keepdims=True)

        spread = (upright(expert) == lane).astype(jnp.bfloat16)
        share_here = upright(experts + expert)
        own = step == 0 and not other

        def merge(span):
            block = done[source, column, :, span] if own else back_in[source, column, :, span]
            term = share_here * jnp.dot(spread, block, preferred_element_type=jnp.float32)
            if own:
                total[:, span] = term
            elif step == line - 1 and other:
                out_ref[:, span] = (total[:, span] + term).astype(jnp.bfloat16)
            else:
                total[:, span] = total[:, span] + term

        for i in range(PARTS):
            if not own:
                back_arrival(source, column, i).wait_recv()
            over_width(i, merge)

    for tick in range(line + 1):
        if tick < line:
            dispatch(tick)
        if tick:
            compute(tick - 1)
            finish(tick - 1)
        if tick < line:
            forward(tick)
    for step in range(line):
        gather(step, False)
        gather(step, True)
    for step in range(line):
        source = order(step)
        if step:
            meta_copy(step).wait_send()
        for i in range(PARTS):
            hops(source, i, lambda copy: copy.wait_send())
            back_copy(source, 1 - y, i).wait_send()
            if step:
                back_copy(source, y, i).wait_send()
            cross_copy(source, i).wait_send()
            for column in range(2):
                pair_move(source, core, column, i).wait_send()
            part_copy(source, i).wait_send()


def fused(line, tokens, norm_gain, expert_ids, route_weights, gate_proj, linear_proj, down_proj):
    tok_count, width = tokens.shape
    picks = expert_ids.shape[1]
    experts = 2 * line
    capacity = 2 * tok_count * picks // experts
    ff = gate_proj.shape[2]
    wide, dma = jnp.bfloat16, pltpu.SemaphoreType.DMA
    inside, outside = pl.BlockSpec(memory_space=pltpu.VMEM), pl.BlockSpec(memory_space=pl.ANY)
    return pl.pallas_call(
        functools.partial(kernel, line),
        out_shape=jax.ShapeDtypeStruct((tok_count, width), wide),
        in_specs=[inside] * 4 + [outside] * 3,
        out_specs=inside,
        scratch_shapes=[
            pltpu.VMEM((width, ff), wide),
            pltpu.VMEM((width, ff), wide),
            pltpu.VMEM((ff, width), wide),
            pltpu.VMEM((line, tok_count, width), wide),
            pltpu.VMEM((line, 2 * experts, tok_count), jnp.float32),
            pltpu.VMEM((line, 2, 2, capacity, width), wide),
            pltpu.VMEM((line, capacity, width), wide),
            pltpu.VMEM((4 * capacity, ff), wide),
            pltpu.VMEM((line, 2, 2, capacity, width), wide),
            pltpu.VMEM((line, 2, capacity, width), wide),
            pltpu.VMEM((line, 2, capacity, width), wide),
            pltpu.VMEM((line, 2, capacity, width), wide),
            pltpu.VMEM((tok_count, width), jnp.float32),
            dma((3,)),
            dma((line, PARTS, 2)), dma((line, PARTS)),
            dma((line,)), dma((line,)),
            dma((line, PARTS)), dma((line, PARTS)),
            dma((line, 2, PARTS)), dma((line, 2, PARTS)),
            dma((line, PARTS)), dma((line, PARTS)),
            dma((line, 2, PARTS)), dma((line, 2, PARTS)),
        ],
        compiler_params=pltpu.CompilerParams(
            collective_id=0, has_side_effects=True, vmem_limit_bytes=60 * 1024 * 1024
        ),
        name="experts",
    )(
        expert_ids.T, route_weights.T, norm_gain.reshape(1, width), tokens,
        gate_proj[0], linear_proj[0], down_proj[0],
    )


def solution(mesh):
    placed = (
        P(("grp", "ep", "tp"), None),
        P(),
        P(("grp", "ep", "tp"), None),
        P(("grp", "ep", "tp"), None),
        P("ep", None, "tp"),
        P("ep", None, "tp"),
        P("ep", "tp", None),
    )
    along = [device.coords[2] for device in mesh.devices[0, :, 0]]
    line = len(set(along))
    paired = line > 1 and along == [index // 2 for index in range(2 * line)] and mesh.shape["tp"] == 2
    return jax.shard_map(
        functools.partial(fused, line) if paired else shards,
        mesh=mesh,
        in_specs=placed,
        out_specs=P(("grp", "ep", "tp"), None),
        check_vma=False,
    )
```

```python
import functools

import jax
import jax.numpy as jnp
from jax import lax
from jax.experimental import pallas as pl
from jax.experimental.pallas import tpu as pltpu
from jax.sharding import PartitionSpec as P

MESH = pl.DeviceIdType.MESH
PARTS = 2


def shards(tokens, norm_gain, expert_ids, route_weights, gate_proj, linear_proj, down_proj):
    tok_count, width = tokens.shape
    picks = expert_ids.shape[1]
    experts = lax.axis_size("ep")
    capacity = 2 * tok_count * picks // experts
    values = tokens.astype(jnp.float32)
    normed = (
        values * lax.rsqrt(jnp.mean(values * values, axis=-1, keepdims=True) + 1e-06) * norm_gain
    ).astype(jnp.bfloat16)
    flat = expert_ids.reshape(-1)
    onehot = (flat[:, None] == jnp.arange(experts, dtype=jnp.int32)[None, :]).astype(jnp.int32)
    slots = jnp.sum((jnp.cumsum(onehot, axis=0) - 1) * onehot, axis=1)
    where = flat * capacity + slots
    buffer = (
        jnp.zeros((experts * capacity, width), jnp.bfloat16)
        .at[where]
        .set(jnp.repeat(normed, picks, axis=0))
    )
    arrived = lax.all_to_all(buffer, "ep", split_axis=0, concat_axis=0, tiled=True)
    rows = lax.all_gather(arrived, "tp", axis=0, tiled=True)
    gate_pre = jnp.dot(rows, gate_proj[0], preferred_element_type=jnp.float32)
    lin_pre = jnp.dot(rows, linear_proj[0], preferred_element_type=jnp.float32)
    glu = jnp.minimum(gate_pre, 7.0)
    lin = jnp.clip(lin_pre, -7.0, 7.0)
    hidden = (glu * jax.nn.sigmoid(1.702 * glu) * (lin + 1.0)).astype(jnp.bfloat16)
    rows = hidden
    summed = lax.psum_scatter(
        jnp.dot(rows, down_proj[0], preferred_element_type=jnp.float32).astype(jnp.bfloat16),
        "tp",
        scatter_dimension=0,
        tiled=True,
    )
    returned = lax.all_to_all(summed, "ep", split_axis=0, concat_axis=0, tiled=True)
    picked = returned[where].reshape(tok_count, picks, width).astype(jnp.float32)
    return jnp.sum(picked * route_weights[:, :, None], axis=1).astype(jnp.bfloat16)


def kernel(
    line, ids_ref, weights_ref, gain_ref, tokens_ref, gate_hbm, linear_hbm, down_hbm, out_ref,
    gate, linear, down, tok, meta, rows, cross, hidden, part, part_in, done, back_in, total,
    load_sem, tok_send, tok_recv, meta_send, meta_recv, cross_send, cross_recv, pair_send, pair_recv,
    part_send, part_recv, back_send, back_recv,
):
    ep, core = lax.axis_index("ep"), lax.axis_index("tp")
    z, y = ep // 2, ep % 2
    experts = 2 * line
    tok_count, width = tokens_ref.shape
    capacity = rows.shape[3]
    ff = gate.shape[1]
    half = width // PARTS
    cols = [slice(i * half, (i + 1) * half) for i in range(PARTS)]
    at_y = {"ep": z * 2 + 1 - y}
    at_core = {"tp": 1 - core}

    def at_z(other):
        return {"ep": other * 2 + y}

    def remote(source, target, send, recv, device):
        return pltpu.make_async_remote_copy(
            src_ref=source, dst_ref=target, send_sem=send, recv_sem=recv,
            device_id=device, device_id_type=MESH,
        )

    loads = [
        pltpu.make_async_copy(source, target, load_sem.at[i])
        for i, (source, target) in enumerate(((gate_hbm, gate), (linear_hbm, linear), (down_hbm, down)))
    ]
    for load in loads:
        load.start()
    barrier = pltpu.get_barrier_semaphore()
    for step in range(1, experts):
        pl.semaphore_signal(barrier, 1, device_id={"ep": (ep + step) % experts}, device_id_type=MESH)
    pl.semaphore_signal(barrier, 1, device_id=at_core, device_id_type=MESH)

    def normalize(i, _):
        span = pl.ds(pl.multiple_of(i * 32, 32), 32)
        values = tokens_ref[span, :].astype(jnp.float32)
        scale = lax.rsqrt(jnp.mean(values * values, axis=-1, keepdims=True) + 1e-06)
        tok[z, span, :] = (values * scale * gain_ref[...]).astype(jnp.bfloat16)
        return 0

    lax.fori_loop(0, tok_count // 32, normalize, 0)
    names = lax.broadcasted_iota(jnp.int32, (experts, tok_count), 0)
    share = jnp.zeros((experts, tok_count), jnp.float32)
    chosen = jnp.zeros((experts, tok_count), jnp.float32)
    for pick in range(ids_ref.shape[0]):
        same = ids_ref[pick : pick + 1, :] == names
        share = share + jnp.where(same, weights_ref[pick : pick + 1, :], 0.0)
        chosen = chosen + jnp.where(same, 1.0, 0.0)
    first = lax.broadcasted_iota(jnp.int32, (tok_count, tok_count), 0)
    second = lax.broadcasted_iota(jnp.int32, (tok_count, tok_count), 1)
    eye = first == second
    before = jnp.where(first < second, 1.0, 0.0).astype(jnp.bfloat16)
    slots = jnp.dot(chosen.astype(jnp.bfloat16), before, preferred_element_type=jnp.float32)
    meta[z, 0:experts, :] = jnp.where(chosen > 0.5, slots, -1.0)
    meta[z, experts : 2 * experts, :] = share
    pl.semaphore_wait(barrier, experts)

    def meta_copy(step):
        return remote(meta.at[z], meta.at[z], meta_send.at[step], meta_recv.at[z], at_z((z + step) % line))

    def meta_arrival(source):
        return remote(meta.at[source], meta.at[source], meta_send.at[0], meta_recv.at[source], at_z((z + 1) % line))

    for step in range(1, line):
        meta_copy(step).start()

    def order(step):
        found = z
        for place in range(line):
            nearest = sorted(range(line), key=lambda other: (abs(other - place), abs(2 * other - line + 1)))
            found = jnp.where(z == place, nearest[step], found)
        return found if step else z

    def hop(source, i, side):
        block = tok.at[source, :, cols[i]]
        return remote(
            block, block, tok_send.at[source, i, side], tok_recv.at[source, i],
            at_z(lax.rem(z + (1 if side else line - 1), line)),
        )

    def hops(source, i, act):
        @pl.when((source <= z) & (z < line - 1))
        def _():
            act(hop(source, i, 1))

        @pl.when((source >= z) & (z > 0))
        def _():
            act(hop(source, i, 0))

    def cross_copy(source, i):
        return remote(
            cross.at[source, :, cols[i]], rows.at[source, core, y, :, cols[i]],
            cross_send.at[source, i], cross_recv.at[source, i], at_y,
        )

    def cross_arrival(source, i):
        return remote(
            cross.at[source, :, cols[i]], rows.at[source, core, 1 - y, :, cols[i]],
            cross_send.at[source, i], cross_recv.at[source, i], at_y,
        )

    def pair_move(source, owner, column, i):
        block = rows.at[source, owner, column, :, cols[i]]
        return remote(block, block, pair_send.at[source, column, i], pair_recv.at[source, column, i], at_core)

    def part_copy(source, i):
        return remote(
            part.at[source, 1 - core, :, :, cols[i]], part_in.at[source, :, :, cols[i]],
            part_send.at[source, i], part_recv.at[source, i], at_core,
        )

    def back_copy(source, column, i):
        return remote(
            done.at[source, column, :, cols[i]], back_in.at[z, y, :, cols[i]],
            back_send.at[source, column, i], back_recv.at[z, y, i], {"ep": source * 2 + column},
        )

    def back_arrival(source, column, i):
        return remote(
            done.at[source, column, :, cols[i]], back_in.at[source, column, :, cols[i]],
            back_send.at[source, column, i], back_recv.at[source, column, i], {"ep": source * 2 + column},
        )

    tile = 512

    def over_width(i, act):
        def go(j, _):
            act(pl.ds(pl.multiple_of(i * half + j * tile, tile), tile))
            return 0

        lax.fori_loop(0, half // tile, go, 0)

    def arrive(tick, i):
        if tick == 0:
            hops(z, i, lambda copy: copy.start())
        for step in range(max(tick, 1), line):
            source = order(step)
            apart = jnp.where(source > z, source - z, z - source)

            @pl.when(apart == tick)
            def _():
                hop(source, i, 0).wait_recv()
                hops(source, i, lambda copy: copy.start())

    def dispatch(step):
        source = order(step)
        place = lax.broadcasted_iota(jnp.int32, (capacity, tok_count), 0).astype(jnp.float32)
        if step:
            meta_arrival(source).wait_recv()
        away = (meta[source, pl.ds(z * 2 + 1 - y, 1), :] == place).astype(jnp.bfloat16)
        here = (meta[source, pl.ds(z * 2 + y, 1), :] == place).astype(jnp.bfloat16)

        def send_away(span):
            cross[source, :, span] = jnp.dot(
                away, tok[source, :, span], preferred_element_type=jnp.float32
            ).astype(jnp.bfloat16)

        def keep_here(span):
            rows[source, core, y, :, span] = jnp.dot(
                here, tok[source, :, span], preferred_element_type=jnp.float32
            ).astype(jnp.bfloat16)

        if step == 0:
            for i in range(PARTS):
                arrive(step, i)
        for i in range(PARTS):
            if step:
                arrive(step, i)
            over_width(i, send_away)
            cross_copy(source, i).start()
            over_width(i, keep_here)
            pair_move(source, core, y, i).start()

    def forward(step):
        source = order(step)
        for i in range(PARTS):
            cross_arrival(source, i).wait_recv()
            pair_move(source, core, 1 - y, i).start()

    def compute(step):
        source = order(step)
        for column in range(2):
            for i in range(PARTS):
                pair_move(source, 1 - core, column, i).wait_recv()
        if step == 0:
            loads[0].wait()
            loads[1].wait()
        depth = 256

        def up(i, _):
            span = pl.ds(pl.multiple_of(i * depth, depth), depth)
            block = rows[source].reshape(4 * capacity, width)
            glu = jnp.minimum(jnp.dot(block, gate[:, span], preferred_element_type=jnp.float32), 7.0)
            lin = jnp.clip(jnp.dot(block, linear[:, span], preferred_element_type=jnp.float32), -7.0, 7.0)
            hidden[:, span] = (glu * jax.nn.sigmoid(1.702 * glu) * (lin + 1.0)).astype(jnp.bfloat16)
            return 0

        lax.fori_loop(0, ff // depth, up, 0)
        if step == 0:
            loads[2].wait()

        def out(span):
            part[source, :, :, :, span] = (
                jnp.dot(hidden[...], down[:, span], preferred_element_type=jnp.float32)
                .astype(jnp.bfloat16)
                .reshape(2, 2, capacity, tile)
            )

        for i in range(PARTS):
            over_width(i, out)
            part_copy(source, i).start()

    def finish(step):
        source = order(step)

        def add(span):
            whole = part[source, core, :, :, span].astype(jnp.float32) + part_in[source, :, :, span].astype(
                jnp.float32
            )
            done[source, :, :, span] = whole.astype(jnp.bfloat16)

        for i in range(PARTS):
            part_copy(source, i).wait_recv()
            over_width(i, add)
            back_copy(source, 1 - y, i).start()
            if step:
                back_copy(source, y, i).start()

    def gather(step, other):
        source, column = order(step), 1 - y if other else y
        expert = source * 2 + column
        lane = lax.broadcasted_iota(jnp.int32, (tok_count, capacity), 1).astype(jnp.float32)

        def upright(row):
            return jnp.sum(jnp.where(eye, meta[z, pl.ds(row, 1), :], 0.0), axis=1, keepdims=True)

        spread = (upright(expert) == lane).astype(jnp.bfloat16)
        share_here = upright(experts + expert)
        own = step == 0 and not other

        def merge(span):
            block = done[source, column, :, span] if own else back_in[source, column, :, span]
            term = share_here * jnp.dot(spread, block, preferred_element_type=jnp.float32)
            if own:
                total[:, span] = term
            elif step == line - 1 and other:
                out_ref[:, span] = (total[:, span] + term).astype(jnp.bfloat16)
            else:
                total[:, span] = total[:, span] + term

        for i in range(PARTS):
            if not own:
                back_arrival(source, column, i).wait_recv()
            over_width(i, merge)

    for tick in range(line + 1):
        if tick < line:
            dispatch(tick)
        if tick:
            compute(tick - 1)
            finish(tick - 1)
        if tick < line:
            forward(tick)
    for step in range(line):
        gather(step, False)
        gather(step, True)
    for step in range(line):
        source = order(step)
        if step:
            meta_copy(step).wait_send()
        for i in range(PARTS):
            hops(source, i, lambda copy: copy.wait_send())
            back_copy(source, 1 - y, i).wait_send()
            if step:
                back_copy(source, y, i).wait_send()
            cross_copy(source, i).wait_send()
            for column in range(2):
                pair_move(source, core, column, i).wait_send()
            part_copy(source, i).wait_send()


def fused(line, tokens, norm_gain, expert_ids, route_weights, gate_proj, linear_proj, down_proj):
    tok_count, width = tokens.shape
    picks = expert_ids.shape[1]
    experts = 2 * line
    capacity = 2 * tok_count * picks // experts
    ff = gate_proj.shape[2]
    wide, dma = jnp.bfloat16, pltpu.SemaphoreType.DMA
    inside, outside = pl.BlockSpec(memory_space=pltpu.VMEM), pl.BlockSpec(memory_space=pl.ANY)
    return pl.pallas_call(
        functools.partial(kernel, line),
        out_shape=jax.ShapeDtypeStruct((tok_count, width), wide),
        in_specs=[inside] * 4 + [outside] * 3,
        out_specs=inside,
        scratch_shapes=[
            pltpu.VMEM((width, ff), wide),
            pltpu.VMEM((width, ff), wide),
            pltpu.VMEM((ff, width), wide),
            pltpu.VMEM((line, tok_count, width), wide),
            pltpu.VMEM((line, 2 * experts, tok_count), jnp.float32),
            pltpu.VMEM((line, 2, 2, capacity, width), wide),
            pltpu.VMEM((line, capacity, width), wide),
            pltpu.VMEM((4 * capacity, ff), wide),
            pltpu.VMEM((line, 2, 2, capacity, width), wide),
            pltpu.VMEM((line, 2, capacity, width), wide),
            pltpu.VMEM((line, 2, capacity, width), wide),
            pltpu.VMEM((line, 2, capacity, width), wide),
            pltpu.VMEM((tok_count, width), jnp.float32),
            dma((3,)),
            dma((line, PARTS, 2)), dma((line, PARTS)),
            dma((line,)), dma((line,)),
            dma((line, PARTS)), dma((line, PARTS)),
            dma((line, 2, PARTS)), dma((line, 2, PARTS)),
            dma((line, PARTS)), dma((line, PARTS)),
            dma((line, 2, PARTS)), dma((line, 2, PARTS)),
        ],
        compiler_params=pltpu.CompilerParams(
            collective_id=0, has_side_effects=True, vmem_limit_bytes=60 * 1024 * 1024
        ),
        name="experts",
    )(
        expert_ids.T, route_weights.T, norm_gain.reshape(1, width), tokens,
        gate_proj[0], linear_proj[0], down_proj[0],
    )


def solution(mesh):
    placed = (
        P(("grp", "ep", "tp"), None),
        P(),
        P(("grp", "ep", "tp"), None),
        P(("grp", "ep", "tp"), None),
        P("ep", None, "tp"),
        P("ep", None, "tp"),
        P("ep", "tp", None),
    )
    along = [device.coords[2] for device in mesh.devices[0, :, 0]]
    line = len(set(along))
    paired = line > 1 and along == [index // 2 for index in range(2 * line)] and mesh.shape["tp"] == 2
    return jax.shard_map(
        functools.partial(fused, line) if paired else shards,
        mesh=mesh,
        in_specs=placed,
        out_specs=P(("grp", "ep", "tp"), None),
        check_vma=False,
    )
```
